32 devices in a mesh: sp: 8 (over z, y), tp: 4 (over x, core).
Axes of the slice: x: 2, y: 2, z: 4, core: 2. Of those that a mesh axis runs over, the one named last changes fastest.
Arguments:
- tokens: bfloat16 [16384, 2048], P('sp'), may hold values from -6 to 6
- w_query: bfloat16 [2048, 1024], P(None, 'tp'), may hold values from -0.125 to 0.125
- w_key: bfloat16 [2048, 1024], P(None, 'tp'), may hold values from -0.125 to 0.125
- w_value: bfloat16 [2048, 1024], P(None, 'tp'), may hold values from -0.125 to 0.125
- w_gate: bfloat16 [2048, 1024], P(None, 'tp'), may hold values from -0.125 to 0.125
- w_pool: bfloat16 [2048, 1024], P(None, 'tp'), may hold values from -0.125 to 0.125
- norm_gain: float32 [1024], P('tp'), may hold values from 0.1 to 1.9
- log_decay: float32 [8, 16384], P('tp', 'sp'), may hold values from -0.8 to 0
- w_out: bfloat16 [2048, 2048], replicated, may hold values from -0.125 to 0.125
Outputs:
- mixed_out: bfloat16 [16384, 2048], P(('sp', 'tp'))
The draws below stay inside these ranges and needn't reach their ends.
All inputs are finite; a program needn't handle non-finite values.
Results may differ from the reference program's by a relative error of at most 0.014.
Values may be sent and summed in bfloat16 or wider, within the bound.
A program may use at most 64 MiB of HBM per device.

```python
import jax
import jax.numpy as jnp
from jax import lax

D = 2048
RETENTION_HEADS = 8
HEAD_DIM = 128
POOL_GROUP = 256
BLOCK = 128
TOK_DEV = 2048
RET_WIDTH = 1024
POOL_WIDTH = 1024
SEQUENCE_TOKENS = 16384


def draw_log_decay(key, part):
    key_perm, key_fast, key_slow, key_dev, key_position, key_level = jax.random.split(jax.random.fold_in(key, 11), 6)
    order = jax.random.permutation(key_perm, RETENTION_HEADS)
    slow_heads = order < RETENTION_HEADS // 2
    fast_rate = jnp.exp(jax.random.uniform(key_fast, (RETENTION_HEADS,), jnp.float32, jnp.log(1.0 / 60.0), jnp.log(1.0 / 25.0)))
    slow_rate = jnp.exp(jax.random.uniform(key_slow, (RETENTION_HEADS,), jnp.float32, jnp.log(0.2), jnp.log(0.5))) / SEQUENCE_TOKENS
    decay_rates = jnp.where(slow_heads, slow_rate, fast_rate)
    n_devices = SEQUENCE_TOKENS // TOK_DEV
    dev_factor = jnp.exp(jax.random.uniform(key_dev, (n_devices,), jnp.float32, -0.69, 0.69))
    factor_row_list = jnp.repeat(dev_factor, TOK_DEV, total_repeat_length=SEQUENCE_TOKENS)
    cluster_position = jax.random.randint(key_position, (RETENTION_HEADS, 2), 0, SEQUENCE_TOKENS)
    cluster_depth = jax.random.uniform(key_level, (RETENTION_HEADS, 2), jnp.float32, -0.6, -0.22)
    matches = (jnp.arange(SEQUENCE_TOKENS)[None, None, :] == cluster_position[:, :, None]).astype(jnp.float32)
    clusters = jnp.sum(matches * cluster_depth[:, :, None], axis=1)
    return -decay_rates[:, None] * factor_row_list[None, :] + clusters


def levels(key, extent, shards, least, top_value):
    gain, own = 1.0, jax.random.fold_in(key, 6)
    for position, parts in shards:
        draws = jnp.exp(jax.random.uniform(jax.random.fold_in(own, position), (parts,), jnp.float32, least / len(shards), top_value / len(shards)))
        gain = gain * jnp.repeat(draws, extent[position] // parts).reshape([-1 if axis == position else 1 for axis in range(len(extent))])
    return gain


def scatter_about(stream_key, shape, spread, reach, pieces=(), kind=jnp.bfloat16):
    loudness = levels(stream_key, shape, pieces, -0.22, 0.18) if pieces else 1.0
    values = jax.random.normal(stream_key, shape, jnp.float32) * spread * loudness
    return jnp.minimum(jnp.maximum(values, -reach), reach).astype(kind)


def setup_inputs(seed: int = 0) -> dict:
    seeds = jax.random.split(jax.random.key(seed), 10)
    return {
        "tokens": scatter_about(seeds[0], (SEQUENCE_TOKENS, D), 1.0, 6.0, ((0, 8),)),
        "w_query": scatter_about(seeds[1], (D, RET_WIDTH), D ** -0.5, 0.125, ((1, 4),)),
        "w_key": scatter_about(seeds[2], (D, RET_WIDTH), D ** -0.5, 0.125, ((1, 4),)),
        "w_value": scatter_about(seeds[3], (D, RET_WIDTH), D ** -0.5, 0.125, ((1, 4),)),
        "w_gate": scatter_about(seeds[4], (D, RET_WIDTH), D ** -0.5, 0.125, ((1, 4),)),
        "w_pool": scatter_about(seeds[5], (D, POOL_WIDTH), D ** -0.5, 0.125, ((1, 4),)),
        "norm_gain": jnp.clip(1.0 + 0.18 * jax.random.normal(seeds[6], (RET_WIDTH,), jnp.float32), 0.1, 1.9),
        "log_decay": draw_log_decay(jax.random.fold_in(seeds[9], 71), 0),
        "w_out": scatter_about(seeds[8], (RET_WIDTH + POOL_WIDTH, D), (RET_WIDTH + POOL_WIDTH) ** -0.5, 0.125),
    }


def rotate(tensor, positions):
    half_dim = tensor.shape[-1] // 2
    inverse = 10000.0 ** (-jnp.arange(half_dim, dtype=jnp.float32) / half_dim)
    angles = positions.astype(jnp.float32)[:, None] * inverse[None, :]
    cosine = jnp.cos(angles)[:, None, :]
    sine_part = jnp.sin(angles)[:, None, :]
    first_half = tensor[..., :half_dim]
    second_half = tensor[..., half_dim:]
    return jnp.concatenate([first_half * cosine - second_half * sine_part, first_half * sine_part + second_half * cosine], axis=-1)

def block_parts(q_blocks, k_blocks, v_blocks, decay_blocks):
    log_cum = jnp.cumsum(decay_blocks, axis=1)
    block_ends = log_cum[:, -1, :]
    steps_len = q_blocks.shape[1]
    causal = jnp.arange(steps_len)[:, None] >= jnp.arange(steps_len)[None, :]
    head_cum = jnp.transpose(log_cum, (0, 2, 1))
    log_gap = head_cum[:, :, :, None] - head_cum[:, :, None, :]
    weights = jnp.where(causal[None, None], jnp.exp(jnp.minimum(log_gap, 0.0)), 0.0)
    scores = jnp.einsum('nthd,nshd->nhts', q_blocks.astype(jnp.float32), k_blocks.astype(jnp.float32))
    mixing = (scores * weights).astype(jnp.bfloat16)
    inner_part = jnp.einsum('nhts,nshe->nthe', mixing.astype(jnp.float32), v_blocks.astype(jnp.float32))
    keys_decayed = (k_blocks.astype(jnp.float32) * jnp.exp(block_ends[:, None, :] - log_cum)[..., None]).astype(jnp.bfloat16)
    updates = jnp.einsum('nshd,nshe->nhde', keys_decayed.astype(jnp.float32), v_blocks.astype(jnp.float32))
    return (log_cum, block_ends, inner_part, updates)

def reference(tokens, w_query, w_key, w_value, w_gate, w_pool, norm_gain, log_decay, w_out):

    def project(weights):
        return jnp.dot(tokens, weights, preferred_element_type=jnp.float32).astype(jnp.bfloat16)
    query = project(w_query)
    keys_raw = project(w_key)
    values = project(w_value)
    gate_pre = project(w_gate)
    pool_in = project(w_pool)
    positions = jnp.arange(SEQUENCE_TOKENS)
    head_shape = (SEQUENCE_TOKENS, RETENTION_HEADS, HEAD_DIM)
    q_rot = rotate(query.astype(jnp.float32).reshape(head_shape), positions).astype(jnp.bfloat16)
    k_rot = (rotate(keys_raw.astype(jnp.float32).reshape(head_shape), positions) * HEAD_DIM ** (-0.5)).astype(jnp.bfloat16)
    n_blocks = SEQUENCE_TOKENS // BLOCK
    block_shape = (n_blocks, BLOCK, RETENTION_HEADS, HEAD_DIM)
    q_blocks = q_rot.reshape(block_shape)
    k_blocks = k_rot.reshape(block_shape)
    v_blocks = values.reshape(block_shape)
    decay_blocks = jnp.transpose(log_decay).reshape(n_blocks, BLOCK, RETENTION_HEADS)
    log_cum, block_ends, inner_part, updates = block_parts(q_blocks, k_blocks, v_blocks, decay_blocks)

    def advance(running, element):
        block_end, update_n = element
        return (running * jnp.exp(block_end)[:, None, None] + update_n, running)
    zero_state = jnp.zeros((RETENTION_HEADS, HEAD_DIM, HEAD_DIM), jnp.float32)
    _, before_state = lax.scan(advance, zero_state, (block_ends, updates))
    state_bf = lax.optimization_barrier(before_state.astype(jnp.bfloat16))
    cross_part = jnp.einsum('nthd,nhde->nthe', q_blocks.astype(jnp.float32), state_bf.astype(jnp.float32)) * jnp.exp(log_cum)[..., None]
    retained = (inner_part + cross_part).reshape(head_shape)
    centered = retained - lax.optimization_barrier(jnp.mean(retained, axis=-1, keepdims=True))
    normed = centered * lax.rsqrt(lax.optimization_barrier(jnp.mean(centered * centered, axis=-1, keepdims=True)) + 1e-06)
    gated = (jax.nn.silu(gate_pre.astype(jnp.float32)) * norm_gain * normed.reshape(SEQUENCE_TOKENS, RET_WIDTH)).astype(jnp.bfloat16)
    filled = pool_in.astype(jnp.float32)
    prefix = jnp.concatenate([jnp.zeros((1, POOL_WIDTH), jnp.float32), jnp.cumsum(filled, axis=0)], axis=0)
    col_group = jnp.arange(POOL_WIDTH) // POOL_GROUP
    counts_base = (jnp.arange(SEQUENCE_TOKENS) + 1).astype(jnp.float32)[:, None]
    selected = jnp.zeros((SEQUENCE_TOKENS, POOL_WIDTH), jnp.float32)
    for group_idx in range(4):
        window_len = 2 ** (group_idx + 1)
        lower_sum = jnp.concatenate([jnp.zeros((window_len - 1, POOL_WIDTH), jnp.float32), prefix[:SEQUENCE_TOKENS + 1 - window_len]], axis=0)
        window_mean = (prefix[1:] - lower_sum) / jnp.minimum(counts_base, float(window_len))
        selected = jnp.where((col_group == group_idx)[None, :], window_mean, selected)
    pooled = (selected - filled).astype(jnp.bfloat16)
    result = jnp.dot(gated, w_out[:RET_WIDTH], preferred_element_type=jnp.float32) + jnp.dot(pooled, w_out[RET_WIDTH:], preferred_element_type=jnp.float32)
    return result.astype(jnp.bfloat16)
```

```python
import functools

import jax
import jax.numpy as jnp
import numpy as np
from jax import lax
from jax.experimental import pallas as pl
from jax.experimental.pallas import tpu as pltpu
from jax.sharding import PartitionSpec as P

HEAD_DIM = 128
POOL_GROUP = 256
BLOCK = 128
CHUNK = 256
HALO = 16
F32 = jnp.float32
BF16 = jnp.bfloat16
MESH = pl.DeviceIdType.MESH


def mm(a, b):
    return jnp.dot(a, b, preferred_element_type=F32)


def rotary_tables(n_blocks):
    half = HEAD_DIM // 2
    inverse = 10000.0 ** (-np.arange(half, dtype=np.float64) / half)
    starts = (np.arange(n_blocks) * BLOCK)[:, None] * inverse[None, :]
    offsets = np.arange(BLOCK)[:, None] * inverse[None, :]

    def pair(angles):
        cosine, sine = np.cos(angles), np.sin(angles)
        return (
            np.concatenate([cosine, cosine], 1).astype(np.float32),
            np.concatenate([-sine, sine], 1).astype(np.float32),
        )

    return *pair(starts), *pair(offsets)


def kernel(
    sp_n, tp_n,
    tokens, wq, wk, wv, wg, wp, gain, log_decay, wout, cos_b, sin_b, cos_r, sin_r,
    out,
    tok_v, wq_v, wk_v, wv_v, wg_v, wp_v, wout_v,
    ld_s, cum_s, bend_s, reach_s, col_s,
    k_s, v_s, q_s, g_s, pool_s, inner_s, before_s, state_s,
    st_send, st_recv, tot_send, tot_recv, rim_recv, inc_s,
    pooled_s, gated_s, gath, acc_s,
    tok_sem, w_sem, st_ssem, st_rsem, tot_ssem, tot_rsem, rim_sem, mix_ssem, mix_rsem,
):
    sp = lax.axis_index("sp")
    tp = lax.axis_index("tp")
    rows = tok_v.shape[0]
    heads = k_s.shape[1] // HEAD_DIM
    pool_cols = pool_s.shape[1]
    ret_width = tp_n * heads * HEAD_DIM
    n_blocks = rows // BLOCK
    n_chunks = rows // CHUNK
    per_chunk = CHUNK // BLOCK
    rows_out = rows // tp_n
    pieces = rows_out // CHUNK
    chips = tp_n // 2
    scale = HEAD_DIM ** (-0.5)

    barrier = pltpu.get_barrier_semaphore()

    def load(src, dst, sem):
        return pltpu.make_async_copy(src, dst, sem)

    def tok_copy(c):
        r = pl.ds(pl.multiple_of(c * CHUNK, CHUNK), CHUNK)
        return load(tokens.at[r], tok_v.at[r], tok_sem.at[c])

    load_k = load(wk, wk_v, w_sem.at[0])
    load_v = load(wv, wv_v, w_sem.at[1])
    load_p = load(wp, wp_v, w_sem.at[2])
    load_q = load(wq, wq_v, w_sem.at[3])
    load_g = load(wg, wg_v, w_sem.at[4])
    load_o = load(wout, wout_v, w_sem.at[5])
    load_k.start()
    tok_copy(0).start()
    load_v.start()

    def start_tok(c, carry):
        tok_copy(c).start()
        return carry

    lax.fori_loop(1, n_chunks, start_tok, 0)
    load_p.start()

    def greet_sp(d, carry):
        pl.semaphore_signal(barrier, inc=1, device_id=((sp + d) % sp_n, tp), device_id_type=MESH)
        return carry

    def greet_tp(d, carry):
        pl.semaphore_signal(barrier, inc=1, device_id=(sp, (tp + d) % tp_n), device_id_type=MESH)
        return carry

    lax.fori_loop(1, sp_n, greet_sp, 0)
    lax.fori_loop(1, tp_n, greet_tp, 0)

    for n in range(n_blocks):
        ld_s[n * heads : (n + 1) * heads, :] = log_decay[:, n * BLOCK : (n + 1) * BLOCK]
    t_iota = lax.broadcasted_iota(jnp.int32, (BLOCK, BLOCK), 0)
    s_iota = lax.broadcasted_iota(jnp.int32, (BLOCK, BLOCK), 1)
    causal = t_iota >= s_iota
    upper = jnp.where(t_iota <= s_iota, 1.0, 0.0).astype(F32)
    ld = ld_s[...]
    cum_s[...] = jnp.dot(ld, upper, preferred_element_type=F32, precision=lax.Precision.HIGHEST)
    bend_s[...] = jnp.dot(
        ld, jnp.ones((BLOCK, BLOCK), F32), preferred_element_type=F32,
        precision=lax.Precision.HIGHEST,
    )
    run = jnp.zeros((heads, HEAD_DIM), F32)
    for n in range(n_blocks):
        reach_s[n * heads : (n + 1) * heads, :] = jnp.exp(run)
        run = run + bend_s[n * heads : (n + 1) * heads, :]
    tot_send[...] = jnp.zeros_like(tot_send)
    tot_send[0:heads, :] = jnp.exp(run)
    state_s[...] = jnp.zeros_like(state_s)
    load_k.wait()
    load_v.wait()

    def angles(n):
        at = pl.ds(sp * n_blocks + n, 1)
        cb, sb = cos_b[at, :], sin_b[at, :]
        cr, sr = cos_r[...], sin_r[...]
        return cb * cr - sb * sr, sb * cr + cb * sr

    def turned(x, cosine, sine):
        return x * cosine + pltpu.roll(x, HEAD_DIM // 2, 1) * sine

    def chunk_rows(c):
        return pl.ds(pl.multiple_of(c * CHUNK, CHUNK), CHUNK)

    def block_rows(n):
        return pl.ds(pl.multiple_of(n * BLOCK, BLOCK), BLOCK)

    def kv_chunk(c, carry):
        tok_copy(c).wait()
        x = tok_v[chunk_rows(c), :]
        key = mm(x, wk_v[...]).astype(BF16).astype(F32)
        value = mm(x, wv_v[...]).astype(BF16)
        v_s[chunk_rows(c), :] = value
        for b in range(per_chunk):
            n = c * per_chunk + b
            cosine, sine = angles(n)
            for h in range(heads):
                cols = slice(h * HEAD_DIM, (h + 1) * HEAD_DIM)
                part = slice(b * BLOCK, (b + 1) * BLOCK)
                k_rot = (turned(key[part, cols], cosine, sine) * scale).astype(BF16)
                k_s[block_rows(n), cols] = k_rot
                at = n * heads + h
                col = jnp.broadcast_to(cum_s[pl.ds(at, 1), :], (BLOCK, BLOCK)).T
                col_s[at] = col
                end = bend_s[pl.ds(at, 1), :]
                decayed = (k_rot.astype(F32) * jnp.exp(end - col)).astype(BF16)
                update = lax.dot_general(
                    decayed, value[part, cols], (((0,), (0,)), ((), ())),
                    preferred_element_type=F32,
                )
                state = state_s[h]
                before_s[at] = state
                state_s[h] = state * jnp.exp(end) + update
        return carry

    lax.fori_loop(0, n_chunks, kv_chunk, 0)
    load_q.start()
    load_g.start()
    load_o.start()
    for h in range(heads):
        st_send[h] = state_s[h].astype(BF16)

    pl.semaphore_wait(barrier, sp_n - 1 + tp_n - 1)

    def state_copies(d):
        target = ((sp + d) % sp_n, tp)
        return (
            pltpu.make_async_remote_copy(
                src_ref=tot_send, dst_ref=tot_recv.at[sp], send_sem=tot_ssem.at[d],
                recv_sem=tot_rsem.at[sp], device_id=target, device_id_type=MESH,
            ),
            pltpu.make_async_remote_copy(
                src_ref=st_send, dst_ref=st_recv.at[sp], send_sem=st_ssem.at[d],
                recv_sem=st_rsem.at[sp], device_id=target, device_id_type=MESH,
            ),
        )

    def send_state(d, carry):
        for copy in state_copies(d):
            copy.start()
        return carry

    def sent_state(d, carry):
        for copy in state_copies(d):
            copy.wait_send()
        return carry

    lax.fori_loop(1, sp_n - sp, send_state, 0)

    load_p.wait()

    def pool_chunk(c):
        at = pl.ds(pl.multiple_of(HALO + c * CHUNK, HALO), CHUNK)
        pool_s[at, :] = mm(tok_v[chunk_rows(c), :], wp_v[...]).astype(BF16)

    pool_chunk(n_chunks - 1)
    rim = pltpu.make_async_remote_copy(
        src_ref=pool_s.at[pl.ds(rows, HALO)], dst_ref=rim_recv, send_sem=rim_sem.at[0],
        recv_sem=rim_sem.at[1], device_id=((sp + 1) % sp_n, tp), device_id_type=MESH,
    )

    @pl.when(sp < sp_n - 1)
    def _():
        rim.start()

    def pool_step(c, carry):
        pool_chunk(c)
        return carry

    lax.fori_loop(0, n_chunks - 1, pool_step, 0)

    @pl.when(sp == 0)
    def _():
        pool_s[0:HALO, :] = jnp.zeros((HALO, pool_cols), BF16)

    @pl.when(sp > 0)
    def _():
        rim.wait_recv()
        pool_s[0:HALO, :] = rim_recv[...]

    def target_of(t):
        chip = (tp // 2 + 1 + t // (2 * pieces)) % chips
        piece = (t % (2 * pieces)) // 2
        dest = chip * 2 + (tp + t + 1) % 2
        return dest, piece, dest * pieces + piece

    def mix_copy(kind, t):
        dest, piece, c = target_of(t)
        src = (gated_s, pooled_s)[kind]
        width = src.shape[1]
        first = pl.multiple_of(kind * ret_width + tp * width, HEAD_DIM)
        return pltpu.make_async_remote_copy(
            src_ref=src.at[chunk_rows(c)],
            dst_ref=gath.at[chunk_rows(piece), pl.ds(first, width)],
            send_sem=mix_ssem.at[kind, t],
            recv_sem=mix_rsem.at[kind, tp, piece],
            device_id=(sp, dest), device_id_type=MESH,
        )

    def hand_over(kind, t, block):
        dest, piece, c = target_of(t)
        dst = (gated_s, pooled_s)[kind]
        width = dst.shape[1]
        first = pl.multiple_of(kind * ret_width + tp * width, HEAD_DIM)

        @pl.when(dest == tp)
        def _():
            gath[chunk_rows(piece), pl.ds(first, width)] = block

        @pl.when(dest != tp)
        def _():
            dst[chunk_rows(c), :] = block
            mix_copy(kind, t).start()

    group = (tp * pool_cols) // POOL_GROUP
    window = lax.shift_left(jnp.int32(2), group.astype(jnp.int32))
    gap = (
        lax.broadcasted_iota(jnp.int32, (CHUNK, CHUNK + HALO), 0)
        + HALO
        - lax.broadcasted_iota(jnp.int32, (CHUNK, CHUNK + HALO), 1)
    )
    band = jnp.where((gap >= 0) & (gap < window), 1.0, 0.0).astype(BF16)
    row_iota = lax.broadcasted_iota(jnp.int32, (CHUNK, pool_cols), 0)

    def pool_send(t, carry):
        _, _, c = target_of(t)
        at = pl.ds(pl.multiple_of(c * CHUNK, CHUNK), CHUNK + HALO)
        sums = mm(band, pool_s[at, :])
        own = pool_s[pl.ds(pl.multiple_of(HALO + c * CHUNK, HALO), CHUNK), :].astype(F32)
        count = jnp.minimum(sp * rows + c * CHUNK + row_iota + 1, window).astype(F32)
        hand_over(1, t, (sums / count - own).astype(BF16))
        return carry

    lax.fori_loop(0, n_chunks, pool_send, 0)

    load_q.wait()
    load_g.wait()

    def q_chunk(c, carry):
        x = tok_v[chunk_rows(c), :]
        query = mm(x, wq_v[...]).astype(BF16).astype(F32)
        g_s[chunk_rows(c), :] = mm(x, wg_v[...]).astype(BF16)
        for b in range(per_chunk):
            n = c * per_chunk + b
            cosine, sine = angles(n)
            for h in range(heads):
                cols = slice(h * HEAD_DIM, (h + 1) * HEAD_DIM)
                q_rot = turned(query[b * BLOCK : (b + 1) * BLOCK, cols], cosine, sine).astype(BF16)
                q_s[block_rows(n), cols] = q_rot
                at = n * heads + h
                fade = jnp.exp(jnp.minimum(col_s[at] - cum_s[pl.ds(at, 1), :], 0.0))
                scores = lax.dot_general(
                    q_rot, k_s[block_rows(n), cols], (((1,), (1,)), ((), ())),
                    preferred_element_type=F32,
                )
                mixing = (scores * jnp.where(causal, fade, 0.0)).astype(BF16)
                inner_s[block_rows(n), cols] = mm(mixing, v_s[block_rows(n), cols])
        return carry

    lax.fori_loop(0, n_chunks, q_chunk, 0)

    inc_s[...] = jnp.zeros_like(inc_s)

    def enter(i, carry):
        tot_in = pltpu.make_async_copy(tot_recv.at[i], tot_recv.at[i], tot_rsem.at[i])
        st_in = pltpu.make_async_copy(st_recv.at[i], st_recv.at[i], st_rsem.at[i])
        tot_in.wait()
        st_in.wait()
        for h in range(heads):
            inc_s[h] = inc_s[h] * tot_recv[i, h : h + 1, :] + st_recv[i, h].astype(F32)
        return carry

    lax.fori_loop(0, sp, enter, 0)

    def ret_send(t, carry):
        _, _, c = target_of(t)
        parts = []
        for b in range(per_chunk):
            n = c * per_chunk + b
            line = []
            for h in range(heads):
                cols = slice(h * HEAD_DIM, (h + 1) * HEAD_DIM)
                at = n * heads + h
                state = (before_s[at] + reach_s[pl.ds(at, 1), :] * inc_s[h]).astype(BF16)
                cross = mm(q_s[block_rows(n), cols], state) * jnp.exp(col_s[at])
                kept = inner_s[block_rows(n), cols] + cross
                centered = kept - jnp.mean(kept, axis=-1, keepdims=True)
                power = jnp.mean(centered * centered, axis=-1, keepdims=True)
                normed = centered * lax.rsqrt(power + 1e-06)
                gate = g_s[block_rows(n), cols].astype(F32)
                line.append((jax.nn.silu(gate) * gain[:, cols] * normed).astype(BF16))
            parts.append(jnp.concatenate(line, axis=1) if heads > 1 else line[0])
        hand_over(0, t, jnp.concatenate(parts, axis=0))
        return carry

    lax.fori_loop(0, n_chunks, ret_send, 0)

    load_o.wait()

    def arrived(kind, src, piece):
        width = (gated_s, pooled_s)[kind].shape[1]
        here = gath.at[
            chunk_rows(piece), pl.ds(pl.multiple_of(kind * ret_width + src * width, HEAD_DIM), width)
        ]
        pltpu.make_async_copy(here, here, mix_rsem.at[kind, src, piece]).wait()

    def wait_piece(kind, piece):
        def one(d, carry):
            arrived(kind, (tp + d) % tp_n, piece)
            return carry

        lax.fori_loop(1, tp_n, one, 0)

    width_out = wout_v.shape[1]
    tile = min(512, width_out)

    def tile_cols(j):
        return pl.ds(pl.multiple_of(j * tile, tile), tile)

    def pool_out(piece, carry):
        wait_piece(1, piece)

        def one(j, carry):
            acc_s[chunk_rows(piece), tile_cols(j)] = mm(
                gath[chunk_rows(piece), ret_width:], wout_v[ret_width:, tile_cols(j)]
            )
            return carry

        return lax.fori_loop(0, width_out // tile, one, carry)

    lax.fori_loop(0, pieces, pool_out, 0)

    def ret_out(piece, carry):
        wait_piece(0, piece)

        def one(j, carry):
            total = acc_s[chunk_rows(piece), tile_cols(j)] + mm(
                gath[chunk_rows(piece), :ret_width], wout_v[:ret_width, tile_cols(j)]
            )
            out[chunk_rows(piece), tile_cols(j)] = total.astype(BF16)
            return carry

        return lax.fori_loop(0, width_out // tile, one, carry)

    lax.fori_loop(0, pieces, ret_out, 0)

    lax.fori_loop(1, sp_n - sp, sent_state, 0)

    @pl.when(sp < sp_n - 1)
    def _():
        rim.wait_send()

    def sent_mix(t, carry):
        dest, _, _ = target_of(t)

        @pl.when(dest != tp)
        def _():
            mix_copy(0, t).wait_send()
            mix_copy(1, t).wait_send()

        return carry

    lax.fori_loop(0, n_chunks, sent_mix, 0)


def local(
    sp_n, tp_n, tables, tokens, w_query, w_key, w_value, w_gate, w_pool, norm_gain, log_decay, w_out
):
    rows, width = tokens.shape
    ret_cols = w_query.shape[1]
    pool_cols = w_pool.shape[1]
    heads = ret_cols // HEAD_DIM
    n_blocks = rows // BLOCK
    n_chunks = rows // CHUNK
    rows_out = rows // tp_n
    assert POOL_GROUP % pool_cols == 0 and rows_out % CHUNK == 0 and tp_n % 2 == 0
    both = n_blocks * heads
    tot_rows = -(-heads // 8) * 8
    hbm = pl.BlockSpec(memory_space=pl.ANY)
    vmem = pl.BlockSpec(memory_space=pltpu.VMEM)
    V = pltpu.VMEM
    dma = pltpu.SemaphoreType.DMA
    return pl.pallas_call(
        functools.partial(kernel, sp_n, tp_n),
        name="layer",
        out_shape=jax.ShapeDtypeStruct((rows_out, w_out.shape[1]), BF16),
        in_specs=[hbm] * 6 + [vmem] * 2 + [hbm] + [vmem] * 4,
        out_specs=vmem,
        scratch_shapes=[
            V((rows, width), BF16),
            V((width, ret_cols), BF16),
            V((width, ret_cols), BF16),
            V((width, ret_cols), BF16),
            V((width, ret_cols), BF16),
            V((width, pool_cols), BF16),
            V(w_out.shape, BF16),
            V((both, BLOCK), F32),
            V((both, BLOCK), F32),
            V((both, BLOCK), F32),
            V((both, BLOCK), F32),
            V((both, BLOCK, BLOCK), F32),
            V((rows, ret_cols), BF16),
            V((rows, ret_cols), BF16),
            V((rows, ret_cols), BF16),
            V((rows, ret_cols), BF16),
            V((HALO + rows, pool_cols), BF16),
            V((rows, ret_cols), F32),
            V((both, HEAD_DIM, HEAD_DIM), F32),
            V((heads, HEAD_DIM, HEAD_DIM), F32),
            V((heads, HEAD_DIM, HEAD_DIM), BF16),
            V((sp_n, heads, HEAD_DIM, HEAD_DIM), BF16),
            V((tot_rows, HEAD_DIM), F32),
            V((sp_n, tot_rows, HEAD_DIM), F32),
            V((HALO, pool_cols), BF16),
            V((heads, HEAD_DIM, HEAD_DIM), F32),
            V((rows, pool_cols), BF16),
            V((rows, ret_cols), BF16),
            V((rows_out, tp_n * (ret_cols + pool_cols)), BF16),
            V((rows_out, w_out.shape[1]), F32),
            dma((n_chunks,)),
            dma((6,)),
            dma((sp_n,)),
            dma((sp_n,)),
            dma((sp_n,)),
            dma((sp_n,)),
            dma((2,)),
            dma((2, n_chunks)),
            dma((2, tp_n, rows_out // CHUNK)),
        ],
        compiler_params=pltpu.CompilerParams(
            collective_id=0, has_side_effects=True, vmem_limit_bytes=62 * 1024 * 1024
        ),
    )(
        tokens, w_query, w_key, w_value, w_gate, w_pool, norm_gain.reshape(1, ret_cols), log_decay,
        w_out, *(jnp.asarray(t) for t in tables),
    )


def solution(mesh):
    sp_n, tp_n = mesh.shape["sp"], mesh.shape["tp"]

    def whole(tokens, *rest):
        tables = rotary_tables(tokens.shape[0] // BLOCK)
        body = functools.partial(local, sp_n, tp_n, tables)
        return jax.shard_map(
            body, mesh=mesh, in_specs=in_specs, out_specs=out_specs, check_vma=False
        )(tokens, *rest)

    in_specs = (
        P("sp", None),
        P(None, "tp"),
        P(None, "tp"),
        P(None, "tp"),
        P(None, "tp"),
        P(None, "tp"),
        P("tp"),
        P("tp", "sp"),
        P(),
    )
    out_specs = P(("sp", "tp"), None)
    return whole
```

```python
import functools

import jax
import jax.numpy as jnp
import numpy as np
from jax import lax
from jax.experimental import pallas as pl
from jax.experimental.pallas import tpu as pltpu
from jax.sharding import PartitionSpec as P

HEAD_DIM = 128
POOL_GROUP = 256
BLOCK = 128
CHUNK = 256
HALO = 16
F32 = jnp.float32
BF16 = jnp.bfloat16
MESH = pl.DeviceIdType.MESH


def mm(a, b):
    return jnp.dot(a, b, preferred_element_type=F32)


def rotary_tables(n_blocks):
    half = HEAD_DIM // 2
    inverse = 10000.0 ** (-np.arange(half, dtype=np.float64) / half)
    starts = (np.arange(n_blocks) * BLOCK)[:, None] * inverse[None, :]
    offsets = np.arange(BLOCK)[:, None] * inverse[None, :]

    def pair(angles):
        cosine, sine = np.cos(angles), np.sin(angles)
        return (
            np.concatenate([cosine, cosine], 1).astype(np.float32),
            np.concatenate([-sine, sine], 1).astype(np.float32),
        )

    return *pair(starts), *pair(offsets)


def kernel(
    sp_n, tp_n,
    tokens, wq, wk, wv, wg, wp, gain, log_decay, wout, cos_b, sin_b, cos_r, sin_r,
    out,
    tok_v, wq_v, wk_v, wv_v, wg_v, wp_v, wout_v,
    ld_s, cum_s, bend_s, reach_s, col_s,
    k_s, v_s, q_s, g_s, kr_s, qr_s, pool_s, inner_s, before_s, state_s,
    st_send, st_recv, tot_send, tot_recv, rim_recv, inc_s,
    pooled_s, gated_s, gath, acc_s,
    tok_sem, w_sem, st_ssem, st_rsem, tot_ssem, tot_rsem, rim_sem, mix_ssem, mix_rsem,
):
    sp = lax.axis_index("sp")
    tp = lax.axis_index("tp")
    rows = tok_v.shape[0]
    heads = k_s.shape[1] // HEAD_DIM
    pool_cols = pool_s.shape[1]
    ret_width = tp_n * heads * HEAD_DIM
    n_blocks = rows // BLOCK
    n_chunks = rows // CHUNK
    per_chunk = CHUNK // BLOCK
    rows_out = rows // tp_n
    pieces = rows_out // CHUNK
    chips = tp_n // 2
    scale = HEAD_DIM ** (-0.5)

    barrier = pltpu.get_barrier_semaphore()

    def load(src, dst, sem):
        return pltpu.make_async_copy(src, dst, sem)

    def tok_copy(c):
        r = pl.ds(pl.multiple_of(c * CHUNK, CHUNK), CHUNK)
        return load(tokens.at[r], tok_v.at[r], tok_sem.at[c])

    load_k = load(wk, wk_v, w_sem.at[0])
    load_v = load(wv, wv_v, w_sem.at[1])
    load_p = load(wp, wp_v, w_sem.at[2])
    load_q = load(wq, wq_v, w_sem.at[3])
    load_g = load(wg, wg_v, w_sem.at[4])
    load_o = load(wout, wout_v, w_sem.at[5])
    load_p.start()
    tok_copy(n_chunks - 1).start()
    load_k.start()
    load_v.start()

    def start_tok(c, carry):
        tok_copy(c).start()
        return carry

    lax.fori_loop(0, n_chunks - 1, start_tok, 0)

    def greet_sp(d, carry):
        pl.semaphore_signal(barrier, inc=1, device_id=((sp + d) % sp_n, tp), device_id_type=MESH)
        return carry

    def greet_tp(d, carry):
        pl.semaphore_signal(barrier, inc=1, device_id=(sp, (tp + d) % tp_n), device_id_type=MESH)
        return carry

    lax.fori_loop(1, sp_n, greet_sp, 0)
    lax.fori_loop(1, tp_n, greet_tp, 0)

    for n in range(n_blocks):
        ld_s[n * heads : (n + 1) * heads, :] = log_decay[:, n * BLOCK : (n + 1) * BLOCK]
    t_iota = lax.broadcasted_iota(jnp.int32, (BLOCK, BLOCK), 0)
    s_iota = lax.broadcasted_iota(jnp.int32, (BLOCK, BLOCK), 1)
    causal = t_iota >= s_iota
    upper = jnp.where(t_iota <= s_iota, 1.0, 0.0).astype(F32)
    ld = ld_s[...]
    cum_s[...] = jnp.dot(ld, upper, preferred_element_type=F32, precision=lax.Precision.HIGHEST)
    bend_s[...] = jnp.dot(
        ld, jnp.ones((BLOCK, BLOCK), F32), preferred_element_type=F32,
        precision=lax.Precision.HIGHEST,
    )
    run = jnp.zeros((heads, HEAD_DIM), F32)
    for n in range(n_blocks):
        reach_s[n * heads : (n + 1) * heads, :] = jnp.exp(run)
        run = run + bend_s[n * heads : (n + 1) * heads, :]
    tot_send[...] = jnp.zeros_like(tot_send)
    tot_send[0:heads, :] = jnp.exp(run)
    state_s[...] = jnp.zeros_like(state_s)

    def angles(n):
        at = pl.ds(sp * n_blocks + n, 1)
        cb, sb = cos_b[at, :], sin_b[at, :]
        cr, sr = cos_r[...], sin_r[...]
        return cb * cr - sb * sr, sb * cr + cb * sr

    def turned(x, cosine, sine):
        return x * cosine + pltpu.roll(x, HEAD_DIM // 2, 1) * sine

    def chunk_rows(c):
        return pl.ds(pl.multiple_of(c * CHUNK, CHUNK), CHUNK)

    def block_rows(n):
        return pl.ds(pl.multiple_of(n * BLOCK, BLOCK), BLOCK)

    load_p.wait()
    tok_copy(n_chunks - 1).wait()

    def pool_chunk(c):
        at = pl.ds(pl.multiple_of(HALO + c * CHUNK, HALO), CHUNK)
        pool_s[at, :] = mm(tok_v[chunk_rows(c), :], wp_v[...]).astype(BF16)

    pool_chunk(n_chunks - 1)
    pl.semaphore_wait(barrier, sp_n - 1 + tp_n - 1)
    rim = pltpu.make_async_remote_copy(
        src_ref=pool_s.at[pl.ds(rows, HALO)], dst_ref=rim_recv, send_sem=rim_sem.at[0],
        recv_sem=rim_sem.at[1], device_id=((sp + 1) % sp_n, tp), device_id_type=MESH,
    )

    @pl.when(sp < sp_n - 1)
    def _():
        rim.start()

    load_k.wait()
    load_v.wait()

    step = 2 * CHUNK if rows % (2 * CHUNK) == 0 else CHUNK
    n_steps = rows // step

    def step_rows(c):
        return pl.ds(pl.multiple_of(c * step, step), step)

    def kv_dots(c):
        x = tok_v[step_rows(c), :]
        return mm(x, wk_v[...]).astype(BF16), mm(x, wv_v[...]).astype(BF16)

    def kv_blocks(c):
        key = k_s[step_rows(c), :].astype(F32)
        value = v_s[step_rows(c), :]
        for b in range(step // BLOCK):
            n = c * (step // BLOCK) + b
            cosine, sine = angles(n)
            for h in range(heads):
                cols = slice(h * HEAD_DIM, (h + 1) * HEAD_DIM)
                part = slice(b * BLOCK, (b + 1) * BLOCK)
                k_rot = (turned(key[part, cols], cosine, sine) * scale).astype(BF16)
                kr_s[block_rows(n), cols] = k_rot
                at = n * heads + h
                col = jnp.broadcast_to(cum_s[pl.ds(at, 1), :], (BLOCK, BLOCK)).T
                col_s[at] = col
                end = bend_s[pl.ds(at, 1), :]
                decayed = (k_rot.astype(F32) * jnp.exp(end - col)).astype(BF16)
                update = lax.dot_general(
                    decayed, value[part, cols], (((0,), (0,)), ((), ())),
                    preferred_element_type=F32,
                )
                state = state_s[h]
                before_s[at] = state
                state_s[h] = state * jnp.exp(end) + update

    def kv_store(c, pair):
        k_s[step_rows(c), :] = pair[0]
        v_s[step_rows(c), :] = pair[1]

    def kv_chunk(c, carry):
        tok_wait(c)
        pair = kv_dots(c)
        kv_blocks(c - 1)
        kv_store(c, pair)
        return carry

    def tok_wait(c):
        for i in range(step // CHUNK):
            at = c * (step // CHUNK) + i

            @pl.when(at < n_chunks - 1)
            def _():
                tok_copy(at).wait()

    tok_wait(0)
    kv_store(0, kv_dots(0))
    lax.fori_loop(1, n_steps, kv_chunk, 0)
    kv_blocks(n_steps - 1)
    load_q.start()
    load_g.start()
    load_o.start()
    for h in range(heads):
        st_send[h] = state_s[h].astype(BF16)

    def state_copies(d):
        target = ((sp + d) % sp_n, tp)
        return (
            pltpu.make_async_remote_copy(
                src_ref=tot_send, dst_ref=tot_recv.at[sp], send_sem=tot_ssem.at[d],
                recv_sem=tot_rsem.at[sp], device_id=target, device_id_type=MESH,
            ),
            pltpu.make_async_remote_copy(
                src_ref=st_send, dst_ref=st_recv.at[sp], send_sem=st_ssem.at[d],
                recv_sem=st_rsem.at[sp], device_id=target, device_id_type=MESH,
            ),
        )

    def send_state(d, carry):
        for copy in state_copies(d):
            copy.start()
        return carry

    def sent_state(d, carry):
        for copy in state_copies(d):
            copy.wait_send()
        return carry

    lax.fori_loop(1, sp_n - sp, send_state, 0)

    def pool_step(c, carry):
        pool_chunk(c)
        return carry

    lax.fori_loop(0, n_chunks - 1, pool_step, 0)

    @pl.when(sp == 0)
    def _():
        pool_s[0:HALO, :] = jnp.zeros((HALO, pool_cols), BF16)

    @pl.when(sp > 0)
    def _():
        rim.wait_recv()
        pool_s[0:HALO, :] = rim_recv[...]

    def target_of(t):
        chip = (tp // 2 + 1 + t // (2 * pieces)) % chips
        piece = (t % (2 * pieces)) // 2
        dest = chip * 2 + (tp + t + 1) % 2
        return dest, piece, dest * pieces + piece

    def mix_copy(kind, t):
        dest, piece, c = target_of(t)
        src = (gated_s, pooled_s)[kind]
        width = src.shape[1]
        first = pl.multiple_of(kind * ret_width + tp * width, HEAD_DIM)
        return pltpu.make_async_remote_copy(
            src_ref=src.at[chunk_rows(c)],
            dst_ref=gath.at[chunk_rows(piece), pl.ds(first, width)],
            send_sem=mix_ssem.at[kind, t],
            recv_sem=mix_rsem.at[kind, tp, piece],
            device_id=(sp, dest), device_id_type=MESH,
        )

    def hand_over(kind, t, block):
        dest, piece, c = target_of(t)
        dst = (gated_s, pooled_s)[kind]
        width = dst.shape[1]
        first = pl.multiple_of(kind * ret_width + tp * width, HEAD_DIM)

        @pl.when(dest == tp)
        def _():
            gath[chunk_rows(piece), pl.ds(first, width)] = block

        @pl.when(dest != tp)
        def _():
            dst[chunk_rows(c), :] = block
            mix_copy(kind, t).start()

    group = (tp * pool_cols) // POOL_GROUP
    window = lax.shift_left(jnp.int32(2), group.astype(jnp.int32))
    gap = (
        lax.broadcasted_iota(jnp.int32, (CHUNK, CHUNK + HALO), 0)
        + HALO
        - lax.broadcasted_iota(jnp.int32, (CHUNK, CHUNK + HALO), 1)
    )
    band = jnp.where((gap >= 0) & (gap < window), 1.0, 0.0).astype(BF16)
    row_iota = lax.broadcasted_iota(jnp.int32, (CHUNK, pool_cols), 0)

    def pool_send(t, carry):
        _, _, c = target_of(t)
        at = pl.ds(pl.multiple_of(c * CHUNK, CHUNK), CHUNK + HALO)
        sums = mm(band, pool_s[at, :])
        own = pool_s[pl.ds(pl.multiple_of(HALO + c * CHUNK, HALO), CHUNK), :].astype(F32)
        count = jnp.minimum(sp * rows + c * CHUNK + row_iota + 1, window).astype(F32)
        hand_over(1, t, (sums / count - own).astype(BF16))
        return carry

    lax.fori_loop(0, n_chunks, pool_send, 0)

    load_q.wait()
    load_g.wait()

    def dest_rows(c):
        return pl.ds(pl.multiple_of(c * rows_out, rows_out), rows_out)

    def q_dots(c):
        x = tok_v[dest_rows(c), :]
        return mm(x, wq_v[...]).astype(BF16), mm(x, wg_v[...]).astype(BF16)

    def q_blocks(c):
        query = q_s[dest_rows(c), :].astype(F32)
        for b in range(rows_out // BLOCK):
            n = c * (rows_out // BLOCK) + b
            cosine, sine = angles(n)
            for h in range(heads):
                cols = slice(h * HEAD_DIM, (h + 1) * HEAD_DIM)
                q_rot = turned(query[b * BLOCK : (b + 1) * BLOCK, cols], cosine, sine).astype(BF16)
                qr_s[block_rows(n), cols] = q_rot
                at = n * heads + h
                fade = jnp.exp(jnp.minimum(col_s[at] - cum_s[pl.ds(at, 1), :], 0.0))
                scores = lax.dot_general(
                    q_rot, kr_s[block_rows(n), cols], (((1,), (1,)), ((), ())),
                    preferred_element_type=F32,
                )
                mixing = (scores * jnp.where(causal, fade, 0.0)).astype(BF16)
                inner_s[block_rows(n), cols] = mm(mixing, v_s[block_rows(n), cols])

    def q_store(c, pair):
        q_s[dest_rows(c), :] = pair[0]
        g_s[dest_rows(c), :] = pair[1]

    def chunk_of(t):
        return (tp // 2 + 1 + t // 2) % chips * 2 + (tp + t + 1) % 2

    def q_chunk(t, carry):
        pair = q_dots(chunk_of(t))
        q_blocks(chunk_of(t - 1))
        q_store(chunk_of(t), pair)
        return carry

    def q_range(first, last):
        q_store(chunk_of(first), q_dots(chunk_of(first)))
        lax.fori_loop(first + 1, last, q_chunk, 0)
        q_blocks(chunk_of(last - 1))

    away = n_chunks - 2 * pieces
    q_range(0, tp_n - 2)

    inc_s[...] = jnp.zeros_like(inc_s)

    def enter(i, carry):
        tot_in = pltpu.make_async_copy(tot_recv.at[i], tot_recv.at[i], tot_rsem.at[i])
        st_in = pltpu.make_async_copy(st_recv.at[i], st_recv.at[i], st_rsem.at[i])
        tot_in.wait()
        st_in.wait()
        for h in range(heads):
            inc_s[h] = inc_s[h] * tot_recv[i, h : h + 1, :] + st_recv[i, h].astype(F32)
        return carry

    lax.fori_loop(0, sp, enter, 0)

    def ret_send(t, carry):
        _, _, c = target_of(t)
        parts = []
        for b in range(per_chunk):
            n = c * per_chunk + b
            line = []
            for h in range(heads):
                cols = slice(h * HEAD_DIM, (h + 1) * HEAD_DIM)
                at = n * heads + h
                state = (before_s[at] + reach_s[pl.ds(at, 1), :] * inc_s[h]).astype(BF16)
                cross = mm(qr_s[block_rows(n), cols], state) * jnp.exp(col_s[at])
                kept = inner_s[block_rows(n), cols] + cross
                centered = kept - jnp.mean(kept, axis=-1, keepdims=True)
                power = jnp.mean(centered * centered, axis=-1, keepdims=True)
                normed = centered * lax.rsqrt(power + 1e-06)
                gate = g_s[block_rows(n), cols].astype(F32)
                line.append((jax.nn.silu(gate) * gain[:, cols] * normed).astype(BF16))
            parts.append(jnp.concatenate(line, axis=1) if heads > 1 else line[0])
        hand_over(0, t, jnp.concatenate(parts, axis=0))
        return carry

    lax.fori_loop(0, away, ret_send, 0)
    q_range(tp_n - 2, tp_n)
    lax.fori_loop(away, n_chunks, ret_send, 0)

    load_o.wait()

    def arrived(kind, src, piece):
        width = (gated_s, pooled_s)[kind].shape[1]
        here = gath.at[
            chunk_rows(piece), pl.ds(pl.multiple_of(kind * ret_width + src * width, HEAD_DIM), width)
        ]
        pltpu.make_async_copy(here, here, mix_rsem.at[kind, src, piece]).wait()

    def wait_piece(kind, piece):
        def one(d, carry):
            arrived(kind, (tp + d) % tp_n, piece)
            return carry

        lax.fori_loop(1, tp_n, one, 0)

    width_out = wout_v.shape[1]
    tile = min(512, width_out)

    def tile_cols(j):
        return pl.ds(pl.multiple_of(j * tile, tile), tile)

    for piece in range(pieces):
        wait_piece(1, piece)

    def pool_out(j, carry):
        acc_s[:, tile_cols(j)] = mm(gath[:, ret_width:], wout_v[ret_width:, tile_cols(j)])
        return carry

    lax.fori_loop(0, width_out // tile, pool_out, 0)

    def ret_out(piece, carry):
        wait_piece(0, piece)

        def one(j, carry):
            total = acc_s[chunk_rows(piece), tile_cols(j)] + mm(
                gath[chunk_rows(piece), :ret_width], wout_v[:ret_width, tile_cols(j)]
            )
            out[chunk_rows(piece), tile_cols(j)] = total.astype(BF16)
            return carry

        return lax.fori_loop(0, width_out // tile, one, carry)

    lax.fori_loop(0, pieces, ret_out, 0)

    lax.fori_loop(1, sp_n - sp, sent_state, 0)

    @pl.when(sp < sp_n - 1)
    def _():
        rim.wait_send()

    def sent_mix(t, carry):
        dest, _, _ = target_of(t)

        @pl.when(dest != tp)
        def _():
            mix_copy(0, t).wait_send()
            mix_copy(1, t).wait_send()

        return carry

    lax.fori_loop(0, n_chunks, sent_mix, 0)


def local(
    sp_n, tp_n, tables, tokens, w_query, w_key, w_value, w_gate, w_pool, norm_gain, log_decay, w_out
):
    rows, width = tokens.shape
    ret_cols = w_query.shape[1]
    pool_cols = w_pool.shape[1]
    heads = ret_cols // HEAD_DIM
    n_blocks = rows // BLOCK
    n_chunks = rows // CHUNK
    rows_out = rows // tp_n
    assert POOL_GROUP % pool_cols == 0 and rows_out % CHUNK == 0 and tp_n % 2 == 0
    both = n_blocks * heads
    tot_rows = -(-heads // 8) * 8
    hbm = pl.BlockSpec(memory_space=pl.ANY)
    vmem = pl.BlockSpec(memory_space=pltpu.VMEM)
    V = pltpu.VMEM
    dma = pltpu.SemaphoreType.DMA
    return pl.pallas_call(
        functools.partial(kernel, sp_n, tp_n),
        name="layer",
        out_shape=jax.ShapeDtypeStruct((rows_out, w_out.shape[1]), BF16),
        in_specs=[hbm] * 6 + [vmem] * 2 + [hbm] + [vmem] * 4,
        out_specs=vmem,
        scratch_shapes=[
            V((rows, width), BF16),
            V((width, ret_cols), BF16),
            V((width, ret_cols), BF16),
            V((width, ret_cols), BF16),
            V((width, ret_cols), BF16),
            V((width, pool_cols), BF16),
            V(w_out.shape, BF16),
            V((both, BLOCK), F32),
            V((both, BLOCK), F32),
            V((both, BLOCK), F32),
            V((both, BLOCK), F32),
            V((both, BLOCK, BLOCK), F32),
            V((rows, ret_cols), BF16),
            V((rows, ret_cols), BF16),
            V((rows, ret_cols), BF16),
            V((rows, ret_cols), BF16),
            V((rows, ret_cols), BF16),
            V((rows, ret_cols), BF16),
            V((HALO + rows, pool_cols), BF16),
            V((rows, ret_cols), F32),
            V((both, HEAD_DIM, HEAD_DIM), F32),
            V((heads, HEAD_DIM, HEAD_DIM), F32),
            V((heads, HEAD_DIM, HEAD_DIM), BF16),
            V((sp_n, heads, HEAD_DIM, HEAD_DIM), BF16),
            V((tot_rows, HEAD_DIM), F32),
            V((sp_n, tot_rows, HEAD_DIM), F32),
            V((HALO, pool_cols), BF16),
            V((heads, HEAD_DIM, HEAD_DIM), F32),
            V((rows, pool_cols), BF16),
            V((rows, ret_cols), BF16),
            V((rows_out, tp_n * (ret_cols + pool_cols)), BF16),
            V((rows_out, w_out.shape[1]), F32),
            dma((n_chunks,)),
            dma((6,)),
            dma((sp_n,)),
            dma((sp_n,)),
            dma((sp_n,)),
            dma((sp_n,)),
            dma((2,)),
            dma((2, n_chunks)),
            dma((2, tp_n, rows_out // CHUNK)),
        ],
        compiler_params=pltpu.CompilerParams(
            collective_id=0, has_side_effects=True, vmem_limit_bytes=62 * 1024 * 1024
        ),
    )(
        tokens, w_query, w_key, w_value, w_gate, w_pool, norm_gain.reshape(1, ret_cols), log_decay,
        w_out, *(jnp.asarray(t) for t in tables),
    )


def solution(mesh):
    sp_n, tp_n = mesh.shape["sp"], mesh.shape["tp"]

    def whole(tokens, *rest):
        tables = rotary_tables(tokens.shape[0] // BLOCK)
        body = functools.partial(local, sp_n, tp_n, tables)
        return jax.shard_map(
            body, mesh=mesh, in_specs=in_specs, out_specs=out_specs, check_vma=False
        )(tokens, *rest)

    in_specs = (
        P("sp", None),
        P(None, "tp"),
        P(None, "tp"),
        P(None, "tp"),
        P(None, "tp"),
        P(None, "tp"),
        P("tp"),
        P("tp", "sp"),
        P(),
    )
    out_specs = P(("sp", "tp"), None)
    return whole
```
